32 devices in a mesh: sp: 8 (over z, x), tp: 4 (over y, core).
Axes of the slice: x: 2, y: 2, z: 4, core: 2. Of those that a mesh axis runs over, the one named last changes fastest.
Arguments:
- resid: bfloat16 [6144, 2048], P(('sp', 'tp')), may hold values from -6 to 6
- queries: bfloat16 [6144, 1024], P('sp', 'tp'), may hold values from -160 to 160
- keys: bfloat16 [6144, 1024], P('sp', 'tp'), may hold values from -6 to 6
- values: bfloat16 [6144, 1024], P('sp', 'tp'), may hold values from -6 to 6
- cum_gate: float32 [6144, 16], P('sp', 'tp'), may hold values from -694 to 0, as said below
- out_weight: bfloat16 [1024, 2048], P('tp'), may hold values from -0.375 to 0.375
- norm_gain: float32 [2048], replicated, may hold values from 0.1 to 1.9
- gate_weight: bfloat16 [2048, 5504], P('sp', 'tp'), may hold values from -0.125 to 0.125
- up_weight: bfloat16 [2048, 5504], P('sp', 'tp'), may hold values from -0.125 to 0.125
- down_weight: bfloat16 [5504, 2048], P('tp', 'sp'), may hold values from -0.078125 to 0.078125
Outputs:
- layer_out: bfloat16 [6144, 2048], P(('sp', 'tp'))
The draws below stay inside these ranges and needn't reach their ends.
Inputs may be any that keep to these rules, and one draw needn't show every extreme that they name: `cum_gate`: each column is non-increasing along positions and starts at or below zero.
All inputs are finite; a program needn't handle non-finite values.
Results may differ from the reference program's by a relative error of at most 0.01.
Values may be sent and summed in bfloat16 or wider, within the bound.
No kernel may reach another device: no remote copies, remote signals or barrier semaphores. Data moves between devices by JAX's collectives and lax.ppermute only.
A program may use at most 256 MiB of HBM per device.

```python
import jax
import jax.numpy as jnp
from jax import lax

D = 2048
HEAD_COUNT = 16
HEAD_DIM = 64
FF = 5504
TOK_DEV = 768
TOKEN_COUNT = 6144
N_SP = 8
N_TP = 4


def paired_rows(key):
    key_query, key_key = jax.random.split(jax.random.fold_in(key, 11))
    width = HEAD_COUNT * HEAD_DIM
    queries = 2.5 * jnp.clip(jax.random.normal(key_query, (TOKEN_COUNT, width), jnp.float32), -5.0, 5.0)
    keys = jnp.clip(jax.random.normal(key_key, (TOKEN_COUNT, width), jnp.float32), -5.0, 5.0)
    return (queries, keys)


def draw_queries(key, part):
    return paired_rows(key)[0].astype(jnp.bfloat16)


def draw_keys(key, part):
    return paired_rows(key)[1].astype(jnp.bfloat16)


def draw_cum_gate(key, part):
    key_fast, key_block, key_rough, key_index_offset, key_length = jax.random.split(jax.random.fold_in(key, 23), 5)
    fast = jax.random.randint(key_fast, (HEAD_COUNT,), 0, 2).astype(jnp.float32)
    blocks = TOKEN_COUNT // TOK_DEV
    block_factor = jnp.exp(jax.random.uniform(key_block, (blocks, 1), jnp.float32, 0.0, jnp.log(3.0)))
    block_factor = jnp.repeat(block_factor, TOK_DEV, axis=0)
    rough = jax.random.uniform(key_rough, (TOKEN_COUNT, HEAD_COUNT), jnp.float32, 0.5, 1.5)
    base = fast * (1.0 / 40.0) + (1.0 - fast) * (0.6 / TOKEN_COUNT)
    stride_offset = -base[None, :] * block_factor * rough
    group_row_block = jax.random.randint(key_index_offset, (4,), 0, TOKEN_COUNT)
    group_row_count = jnp.log(jax.random.uniform(key_length, (4, HEAD_COUNT), jnp.float32, 0.5, 0.8))
    stride_offset = stride_offset.at[group_row_block].add(group_row_count)
    return jnp.cumsum(stride_offset, axis=0)


def block_scale(key, dims, shards, least, largest):
    def one(dim, parts):
        draws = jax.random.uniform(jax.random.fold_in(jax.random.fold_in(key, 6), dim), (parts,), jnp.float32, least / len(shards), largest / len(shards))
        return jnp.repeat(jnp.exp(draws), dims[dim] // parts).reshape((-1,) + (1,) * (len(dims) - dim - 1))

    factor_of = one(*shards[0])
    for cut in shards[1:]:
        factor_of = factor_of * one(*cut)
    return factor_of


def normal_values(rng, dims, spread, limit, pieces=(), held_as=jnp.bfloat16):
    entries = jax.random.normal(rng, dims, jnp.float32) * spread
    if len(pieces) > 0:
        entries = block_scale(rng, dims, pieces, -0.22, 0.18) * entries
    return jnp.clip(entries, min=-limit, max=limit).astype(held_as)


def setup_inputs(seed: int = 0) -> dict:
    key_of = jax.random.split(jax.random.key(seed), 11)
    resid = normal_values(key_of[0], (TOKEN_COUNT, D), 1.0, 6.0, ((0, 32),))
    queries = draw_queries(jax.random.fold_in(key_of[10], 71), 0)
    keys = draw_keys(jax.random.fold_in(key_of[10], 71), 0)
    values = normal_values(key_of[3], (TOKEN_COUNT, HEAD_COUNT * HEAD_DIM), 1.0, 6.0, ((0, 8), (1, 4)))
    cum_gate = draw_cum_gate(jax.random.fold_in(key_of[10], 71), 0)
    out_weight = normal_values(key_of[5], (HEAD_COUNT * HEAD_DIM, D), (HEAD_COUNT * HEAD_DIM // 4) ** -0.5, 0.375, ((0, 4),))
    norm_gain = jnp.clip(1.0 + 0.18 * jax.random.normal(key_of[6], (D,), jnp.float32), 0.1, 1.9)
    gate_weight = normal_values(key_of[7], (D, FF), D ** -0.5, 0.125, ((0, 8), (1, 4)))
    up_weight = normal_values(key_of[8], (D, FF), D ** -0.5, 0.125, ((0, 8), (1, 4)))
    down_weight = normal_values(key_of[9], (FF, D), FF ** -0.5, 0.078125, ((0, 4), (1, 8)))
    return dict(resid=resid, queries=queries, keys=keys, values=values, cum_gate=cum_gate, out_weight=out_weight, norm_gain=norm_gain, gate_weight=gate_weight, up_weight=up_weight, down_weight=down_weight)


def reference(resid, queries, keys, values, cum_gate, out_weight, norm_gain, gate_weight, up_weight, down_weight):
    width = HEAD_COUNT * HEAD_DIM
    total_len = queries.shape[0]
    scale = HEAD_DIM ** (-0.5)
    key_heads = keys.astype(jnp.float32).reshape(total_len, HEAD_COUNT, HEAD_DIM).transpose(1, 0, 2)
    value_heads = values.astype(jnp.float32).reshape(total_len, HEAD_COUNT, HEAD_DIM).transpose(1, 0, 2)
    key_pos = jnp.arange(total_len, dtype=jnp.int32)
    gate_rows = cum_gate.T

    def block(index):
        start = (index * TOK_DEV).astype(jnp.int32)
        query_block = lax.dynamic_slice_in_dim(queries, start, TOK_DEV, 0).astype(jnp.float32)
        query_block = query_block.reshape(TOK_DEV, HEAD_COUNT, HEAD_DIM).transpose(1, 0, 2)
        gate_block = lax.dynamic_slice_in_dim(cum_gate, start, TOK_DEV, 0).T
        score = jnp.einsum('hqd,hkd->hqk', query_block, key_heads) * scale
        score = score + gate_block[:, :, None] - gate_rows[:, None, :]
        query_pos = start + jnp.arange(TOK_DEV, dtype=jnp.int32)
        score = jnp.where(key_pos[None, None, :] <= query_pos[None, :, None], score, -jnp.inf)
        top = lax.optimization_barrier(jnp.max(score, axis=-1, keepdims=True))
        weight = jnp.exp(score - top)
        total = lax.optimization_barrier(jnp.sum(weight, axis=-1, keepdims=True))
        weight_b = lax.optimization_barrier(weight.astype(jnp.bfloat16)).astype(jnp.float32)
        numer = jnp.einsum('hqk,hkd->hqd', weight_b, value_heads)
        result = (numer / total).transpose(1, 0, 2).reshape(TOK_DEV, width)
        return result.astype(jnp.bfloat16)
    attn = lax.map(block, jnp.arange(N_SP, dtype=jnp.int32)).reshape(total_len, width)
    group = width // N_TP
    proj = jnp.zeros((total_len, D), jnp.float32)
    for index in range(N_TP):
        term = jnp.dot(attn[:, index * group:(index + 1) * group], out_weight[index * group:(index + 1) * group], preferred_element_type=jnp.float32)
        proj = proj + lax.optimization_barrier(term.astype(jnp.bfloat16)).astype(jnp.float32)
    mixed = resid.astype(jnp.float32) + proj
    normed = (mixed * lax.rsqrt(lax.optimization_barrier(jnp.mean(mixed * mixed, axis=-1, keepdims=True)) + 1e-06) * norm_gain).astype(jnp.bfloat16)
    gate = jnp.dot(normed, gate_weight, preferred_element_type=jnp.float32)
    upper = jnp.dot(normed, up_weight, preferred_element_type=jnp.float32)
    hidden = (jax.nn.silu(gate) * upper).astype(jnp.bfloat16)
    hid_group = FF // N_TP
    ffn = jnp.zeros((total_len, D), jnp.float32)
    for index in range(N_TP):
        term = jnp.dot(hidden[:, index * hid_group:(index + 1) * hid_group], down_weight[index * hid_group:(index + 1) * hid_group], preferred_element_type=jnp.float32)
        ffn = ffn + lax.optimization_barrier(term.astype(jnp.bfloat16)).astype(jnp.float32)
    return (mixed + 0.5 * ffn).astype(jnp.bfloat16)
```

```python
import functools
import math

import jax
import jax.numpy as jnp
from jax import lax
from jax.experimental import pallas as pl
from jax.experimental.pallas import tpu as pltpu
from jax.sharding import Mesh, PartitionSpec as P

HEAD_DIM = 64
LANES = 128
BF = jnp.bfloat16
F32 = jnp.float32


def rms_norm(mixed, norm_gain):
    scaled = mixed * lax.rsqrt(jnp.mean(mixed * mixed, axis=-1, keepdims=True) + 1e-06) * norm_gain
    return scaled.astype(BF)


def rounded(term):
    return term.astype(BF).astype(F32)


def flash_kernel(first_ref, q_ref, k_ref, g_ref, v_ref, o_ref, *, heads, chunk):
    block, width = q_ref.shape
    start = first_ref[0] + pl.program_id(0) * block
    full = start // chunk
    lane = lax.broadcasted_iota(jnp.int32, (block, width), 1)
    glane = lax.broadcasted_iota(jnp.int32, (block, LANES), 1)
    queries = q_ref[...]
    scale = HEAD_DIM ** (-0.5)
    ones = jnp.ones((chunk, LANES), BF)
    outs = []
    for head in range(heads):
        mine = (lane >= head * HEAD_DIM) & (lane < (head + 1) * HEAD_DIM)
        q_part = jnp.where(mine, queries.astype(F32) * scale, 0.0).astype(BF)
        g_mine = (glane >= 3 * head) & (glane < 3 * head + 3)
        g_part = jnp.where(g_mine, -1.0, 0.0).astype(BF)
        q_full = jnp.concatenate([q_part, g_part], axis=1)

        def step(index, carry, masked, q_full=q_full):
            best, acc = carry
            at = pl.multiple_of(index * chunk, chunk)
            k_full = jnp.concatenate([k_ref[pl.ds(at, chunk), :], g_ref[pl.ds(at, chunk), :]], axis=1)
            v_full = jnp.concatenate([v_ref[pl.ds(at, chunk), :], ones], axis=1)
            score = lax.dot_general(q_full, k_full, (((1,), (1,)), ((), ())), preferred_element_type=F32)
            if masked:
                q_pos = start + lax.broadcasted_iota(jnp.int32, score.shape, 0)
                k_pos = at + lax.broadcasted_iota(jnp.int32, score.shape, 1)
                score = jnp.where(k_pos <= q_pos, score, -jnp.inf)
            new_best = jnp.maximum(best, jnp.max(score, axis=-1, keepdims=True))
            weight = jnp.exp(score - new_best).astype(BF)
            acc = acc * jnp.exp(best - new_best) + lax.dot_general(
                weight, v_full, (((1,), (0,)), ((), ())), preferred_element_type=F32
            )
            return new_best, acc

        carry = (jnp.full((block, 1), -1e30, F32), jnp.zeros((block, width + LANES), F32))
        carry = lax.fori_loop(0, full, functools.partial(step, masked=False), carry)
        _, acc = step(full, carry, True)
        outs.append((acc[:, :width] / acc[:, width : width + 1]).astype(BF))
    result = outs[0]
    for head in range(1, heads):
        result = jnp.where(lane >= head * HEAD_DIM, outs[head], result)
    o_ref[...] = result


def flash(first, queries, keys_values, gates, heads):
    rows, width = queries.shape
    count = keys_values.shape[0]
    block = math.gcd(rows, 512)
    elements = heads * rows * count
    return pl.pallas_call(
        functools.partial(flash_kernel, heads=heads, chunk=block),
        grid_spec=pltpu.PrefetchScalarGridSpec(
            num_scalar_prefetch=1,
            grid=(rows // block,),
            in_specs=[
                pl.BlockSpec((block, width), lambda i, s: (i, 0)),
                pl.BlockSpec((count, width), lambda i, s: (0, 0)),
                pl.BlockSpec((count, LANES), lambda i, s: (0, 0)),
                pl.BlockSpec((count, width), lambda i, s: (0, 1)),
            ],
            out_specs=pl.BlockSpec((block, width), lambda i, s: (i, 0)),
        ),
        out_shape=jax.ShapeDtypeStruct((rows, width), BF),
        compiler_params=pltpu.CompilerParams(
            dimension_semantics=("arbitrary",), vmem_limit_bytes=40 * 1024 * 1024
        ),
        cost_estimate=pl.CostEstimate(
            flops=elements * 1024, bytes_accessed=4 * count * width * 2, transcendentals=elements
        ),
    )(first, queries, keys_values, gates, keys_values)


def gate_terms(gates):
    high = lax.reduce_precision(gates, 8, 7)
    rest = gates - high
    mid = lax.reduce_precision(rest, 8, 7)
    low = rest - mid
    count, heads = gates.shape
    terms = jnp.stack([high, mid, low], axis=-1).reshape(count, 3 * heads).astype(BF)
    return jnp.pad(terms, ((0, 0), (0, LANES - 3 * heads)))


def pair_exchange(array, axis, concat_axis, size):
    half = array.shape[axis] // size
    halves = [lax.slice_in_dim(array, i * half, (i + 1) * half, axis=axis) for i in range(size)]
    odd = lax.axis_index("x") == 1
    mine = jnp.where(odd, halves[1], halves[0])
    other = jnp.where(odd, halves[0], halves[1])
    got = lax.ppermute(other, "x", [(0, 1), (1, 0)])
    return jnp.concatenate([jnp.where(odd, got, mine), jnp.where(odd, mine, got)], axis=concat_axis)


def swap(array, hop):
    axis, mask = hop
    return lax.ppermute(array, axis, [(i, i ^ mask) for i in range(lax.axis_size(axis))])


def hops_of():
    tp_size = lax.axis_size("tp")
    return [("tp", 1 << i) for i in range(tp_size.bit_length() - 1)] + [("x", 1)]


def orders(count):
    links = list(range(1, count))
    return links, links[::-1]


def gather_rows(own):
    hops = hops_of()
    half = own.shape[1] // 2
    parts = []
    for order, columns in zip(orders(len(hops)), (own[:, :half], own[:, half:])):
        block = columns.reshape((1,) * len(hops) + columns.shape)
        parts.append([block, order])
    for level in range(len(hops) - 1):
        for part in parts:
            at = part[1][level]
            part[0] = jnp.concatenate([part[0], swap(part[0], hops[at])], axis=at)
    both = []
    for block, _ in parts:
        block = jnp.concatenate([block, swap(block, hops[0])], axis=0)
        both.append(block.reshape(-1, half))
    return jnp.concatenate(both, axis=1)


def add(a, b):
    return a.astype(F32) + b.astype(F32)


def scatter_rows(halves, rows):
    hops = hops_of()
    pick = lambda a, at, i: lax.slice_in_dim(a, i, i + 1, axis=at)
    results = []
    parts = []
    for order, columns in zip(orders(len(hops)), halves):
        block = columns.reshape((2,) * len(hops) + (rows, columns.shape[1]))
        parts.append([add(pick(block, 0, 0), swap(pick(block, 0, 1), hops[0])).astype(BF), order])
    for level in range(len(hops) - 1):
        for part in parts:
            at = part[1][level]
            total = add(pick(part[0], at, 0), swap(pick(part[0], at, 1), hops[at]))
            part[0] = total if level == len(hops) - 2 else total.astype(BF)
    return [p[0].reshape(rows, -1) for p in parts]


def gather_groups(piece):
    count = lax.axis_size("tp")
    return [piece] + [swap(piece, ("tp", k)) for k in range(1, count)]


def local(
    resid, queries, keys, values, cum_gate, out_weight, norm_gain, gate_weight, up_weight, down_weight,
    *, pair,
):
    groups = lax.axis_size("tp")
    heads_here = cum_gate.shape[1] // pair
    columns = down_weight.shape[1]
    down_half = pair_exchange(down_weight, 0, 1, pair)
    down_half, stacked = lax.optimization_barrier((down_half, jnp.stack([keys, values, queries])))
    down_first = lax.all_gather(down_half[:, :columns], "z", axis=1, tiled=True)
    packed = lax.all_to_all(stacked, "x", split_axis=2, concat_axis=1, tiled=True)
    query_local = packed[2]
    block_rows, width = query_local.shape
    kv_local = jnp.concatenate([packed[0], packed[1]], axis=1)
    kv_local, down_first = lax.optimization_barrier((kv_local, down_first))
    kv_all = lax.all_gather(kv_local, "z", axis=0, tiled=True)
    gates_all = lax.all_gather(cum_gate, ("z", "x"), axis=0, tiled=True)
    gates_mine = lax.dynamic_slice_in_dim(gates_all, lax.axis_index("x") * heads_here, heads_here, axis=1)
    terms_gate = gate_terms(gates_mine)
    proj_pieces = gather_groups(out_weight)
    up_half = pair_exchange(up_weight, 1, 0, pair)
    gate_half = pair_exchange(gate_weight, 1, 0, pair)
    kv_all, terms_gate, gate_half, up_half, down_half = lax.optimization_barrier(
        (kv_all, terms_gate, gate_half, up_half, down_half)
    )
    gate_all = lax.all_gather(gate_half, "z", axis=0, tiled=True)
    up_all = lax.all_gather(up_half, "z", axis=0, tiled=True)
    down_parts = [down_first, lax.all_gather(down_half[:, columns:], "z", axis=1, tiled=True)]

    lane_pad = -width % LANES
    if lane_pad:
        query_local, key_all, value_all = (
            jnp.pad(a, ((0, 0), (0, lane_pad))) for a in (query_local, kv_all[:, :width], kv_all[:, width:])
        )
        kv_all = jnp.concatenate([key_all, value_all], axis=1)
    first = (lax.axis_index("z") * block_rows).astype(jnp.int32).reshape(1)
    attn = flash(first, query_local, kv_all, terms_gate, heads_here)[:, :width]

    own_rows = lax.all_to_all(attn, ("x", "tp"), split_axis=0, concat_axis=1, tiled=True)
    share = own_rows.shape[0]
    row_groups = own_rows.reshape(share, pair, groups, width)
    mixed = resid.astype(F32)
    for k, piece in enumerate(proj_pieces):
        index = lax.axis_index("tp") ^ k
        rows = lax.dynamic_index_in_dim(row_groups, index, axis=2, keepdims=False).reshape(share, pair * width)
        mixed = mixed + rounded(jnp.dot(rows, piece, preferred_element_type=F32))
    normed_all = gather_rows(rms_norm(mixed, norm_gain))
    gate_sum = jnp.dot(normed_all, gate_all, preferred_element_type=F32)
    up_sum = jnp.dot(normed_all, up_all, preferred_element_type=F32)
    hidden = (jax.nn.silu(gate_sum) * up_sum).astype(BF)
    halves = [jnp.dot(hidden, part, preferred_element_type=F32).astype(BF) for part in down_parts]
    sums = scatter_rows(halves, share)
    starts = range(0, sums[0].shape[1], columns)
    ffn = jnp.concatenate([part[:, i : i + columns] for i in starts for part in sums], axis=1)
    return (mixed + 0.5 * ffn).astype(BF)


def solution(mesh):
    sp, tp = mesh.shape["sp"], mesh.shape["tp"]
    pair = 2
    split = Mesh(mesh.devices.reshape(sp // pair, pair, tp), ("z", "x", "tp"))
    seq = ("z", "x")
    in_specs = (
        P(("z", "x", "tp"), None),
        P(seq, "tp"),
        P(seq, "tp"),
        P(seq, "tp"),
        P(seq, "tp"),
        P("tp", None),
        P(),
        P(seq, "tp"),
        P(seq, "tp"),
        P("tp", seq),
    )
    out_specs = P(("z", "x", "tp"), None)
    return jax.shard_map(
        functools.partial(local, pair=pair), mesh=split, in_specs=in_specs, out_specs=out_specs, check_vma=False
    )
```
